32 devices in a mesh: sp: 16 (over z, y, x), tp: 2 (over core).
Axes of the slice: x: 2, y: 2, z: 4, core: 2. Of those that a mesh axis runs over, the one named last changes fastest.
Arguments:
- tokens: bfloat16 [4096, 2048], P('sp'), may hold values from -6 to 6
- ln_gain: float32 [2048], replicated, may hold values from 0.1 to 1.9
- w_query_attn: bfloat16 [2048, 1024], P('sp', 'tp'), may hold values from -0.125 to 0.125
- w_key_attn: bfloat16 [2048, 1024], P('sp', 'tp'), may hold values from -0.125 to 0.125
- w_value_attn: bfloat16 [2048, 1024], P('sp', 'tp'), may hold values from -0.125 to 0.125
- w_query_delta: bfloat16 [2048, 1024], P('sp', 'tp'), may hold values from -0.125 to 0.125
- w_key_delta: bfloat16 [2048, 1024], P('sp', 'tp'), may hold values from -0.125 to 0.125
- w_value_delta: bfloat16 [2048, 1024], P('sp', 'tp'), may hold values from -0.125 to 0.125
- w_beta: bfloat16 [2048, 8], replicated, may hold values from -0.125 to 0.125
- w_decay: bfloat16 [2048, 8], replicated, may hold values from -0.125 to 0.125
- attn_bias: float32 [16], replicated, may hold values from -13 to 1
- decay_log: float32 [8], replicated, may hold values from -15 to -2
- beta_bias: float32 [8], replicated, may hold values from -7 to 1
- log_decay_extra: float32 [4096, 8], P('sp', 'tp'), may hold values from -0.7 to 0, as said below
- attn_gain: float32 [64], replicated, may hold values from 0.1 to 1.9
- delta_gain: float32 [128], replicated, may hold values from 0.1 to 1.9
- w_out_attn: bfloat16 [1024, 2048], P('tp', 'sp'), may hold values from -0.125 to 0.125
- w_out_delta: bfloat16 [1024, 2048], P('tp', 'sp'), may hold values from -0.125 to 0.125
Outputs:
- mixed_out: bfloat16 [4096, 2048], P(('sp', 'tp'))
The draws below stay inside these ranges and needn't reach their ends.
Inputs may be any that keep to these rules, and one draw needn't show every extreme that they name: `log_decay_extra`: never positive.
All inputs are finite; a program needn't handle non-finite values.
Results may differ from the reference program's by a relative error of at most 0.015.
Values may be sent and summed in bfloat16 or wider, within the bound.
A program may use at most 192 MiB of HBM per device.

```python
import math
import jax
import jax.numpy as jnp
from jax import lax

D = 2048
SB_HEADS = 16
SB_DIM = 64
GDN_HEADS = 8
GDN_DIM = 128
DBLOCK = 64
TOK_DEV = 256
SEQ = 4096
N_SP = 16
N_TP = 2


def draw_attn_bias(key, part):
    perm_key, level_key = jax.random.split(jax.random.fold_in(key, 11))
    ranks = jax.random.permutation(perm_key, SB_HEADS)
    slower = ranks < SB_HEADS // 2
    levels = jax.random.uniform(level_key, (SB_HEADS,), jnp.float32)
    far_reach = -jnp.log(jnp.float32(SEQ)) - 1.5 + 1.5 * levels
    near_reach = -jnp.log(jnp.float32(40.0)) - 1.0 + 2.0 * levels
    return jnp.where(slower, far_reach, near_reach).astype(jnp.float32)


def delta_heads(key):
    perm_key, first_key, second_key = jax.random.split(jax.random.fold_in(key, 23), 3)
    ranks = jax.random.permutation(perm_key, GDN_HEADS)
    slower = ranks < GDN_HEADS // 2
    first_level = jax.random.uniform(first_key, (GDN_HEADS,), jnp.float32)
    second_level = jax.random.uniform(second_key, (GDN_HEADS,), jnp.float32)
    return (slower, first_level, second_level)


def draw_decay_log(key, part):
    slower, first_level, second_level = delta_heads(key)
    slow_rate = jnp.log(0.05 + 0.15 * first_level) - jnp.log(jnp.float32(SEQ))
    fast_rate = jnp.log(0.03 + 0.07 * first_level)
    return jnp.where(slower, slow_rate, fast_rate).astype(jnp.float32)


def draw_beta_bias(key, part):
    slower, first_level, second_level = delta_heads(key)
    return jnp.where(slower, -7.0 + second_level, -1.0 + 2.0 * second_level).astype(jnp.float32)


def draw_log_decay_extra(key, part):
    rate_key, location_key, drop_key = jax.random.split(jax.random.fold_in(key, 37), 3)
    rates = jnp.exp(jax.random.uniform(rate_key, (N_SP, GDN_HEADS), jnp.float32, jnp.log(0.4), jnp.log(1.2))) / SEQ
    base = -jnp.repeat(rates, TOK_DEV, axis=0)
    quarter = SEQ // 4
    spots = jax.random.randint(location_key, (4, GDN_HEADS), 0, quarter)
    spots = spots + (jnp.arange(4, dtype=jnp.int32) * quarter)[:, None]
    drops = jnp.log(jax.random.uniform(drop_key, (4, GDN_HEADS), jnp.float32, 0.5, 0.6))
    positions = jnp.arange(SEQ, dtype=jnp.int32)[:, None]
    result = base
    for which in range(4):
        result = result + jnp.where(positions == spots[which][None, :], drops[which][None, :], 0.0)
    return jnp.maximum(result, -0.7).astype(jnp.float32)


def shard_levels(stream_key, shape, pieces, smallest, largest):
    def one(position, blocks):
        draws = jax.random.uniform(jax.random.fold_in(jax.random.fold_in(stream_key, 6), position), (blocks,), jnp.float32, smallest / len(pieces), largest / len(pieces))
        return jnp.repeat(jnp.exp(draws), shape[position] // blocks).reshape((-1,) + (1,) * (len(shape) - position - 1))

    loudness = one(*pieces[0])
    for cut in pieces[1:]:
        loudness = loudness * one(*cut)
    return loudness


def centred(own_key, dims, scale, most, pieces=(), held_as=jnp.bfloat16):
    factor_of = shard_levels(own_key, dims, pieces, -0.22, 0.18) if pieces else 1.0
    drawn = jax.random.normal(own_key, dims, jnp.float32) * scale * factor_of
    return jnp.minimum(jnp.maximum(drawn, -most), most).astype(held_as)


def setup_inputs(seed: int = 0) -> dict:
    key_list = jax.random.split(jax.random.key(seed), 19)
    tokens = centred(key_list[0], (SEQ, D), 1.0, 6.0, ((0, 16),))
    ln_gain = jnp.clip(1.0 + 0.18 * jax.random.normal(key_list[1], (D,), jnp.float32), 0.1, 1.9)
    w_query_attn = centred(key_list[2], (D, SB_HEADS * SB_DIM), D ** -0.5, 0.125, ((0, 16), (1, 2)))
    w_key_attn = centred(key_list[3], (D, SB_HEADS * SB_DIM), D ** -0.5, 0.125, ((0, 16), (1, 2)))
    w_value_attn = centred(key_list[4], (D, SB_HEADS * SB_DIM), D ** -0.5, 0.125, ((0, 16), (1, 2)))
    w_query_delta = centred(key_list[5], (D, GDN_HEADS * GDN_DIM), D ** -0.5, 0.125, ((0, 16), (1, 2)))
    w_key_delta = centred(key_list[6], (D, GDN_HEADS * GDN_DIM), D ** -0.5, 0.125, ((0, 16), (1, 2)))
    w_value_delta = centred(key_list[7], (D, GDN_HEADS * GDN_DIM), D ** -0.5, 0.125, ((0, 16), (1, 2)))
    w_beta = centred(key_list[8], (D, GDN_HEADS), D ** -0.5, 0.125)
    w_decay = centred(key_list[9], (D, GDN_HEADS), D ** -0.5, 0.125)
    attn_bias = draw_attn_bias(jax.random.fold_in(key_list[18], 71), 0)
    decay_log = draw_decay_log(jax.random.fold_in(key_list[18], 71), 0)
    beta_bias = draw_beta_bias(jax.random.fold_in(key_list[18], 71), 0)
    log_decay_extra = draw_log_decay_extra(jax.random.fold_in(key_list[18], 71), 0)
    attn_gain = jnp.clip(1.0 + 0.18 * jax.random.normal(key_list[14], (SB_DIM,), jnp.float32), 0.1, 1.9)
    delta_gain = jnp.clip(1.0 + 0.18 * jax.random.normal(key_list[15], (GDN_DIM,), jnp.float32), 0.1, 1.9)
    w_out_attn = centred(key_list[16], (SB_HEADS * SB_DIM, D), (SB_HEADS * SB_DIM + GDN_HEADS * GDN_DIM) ** -0.5, 0.125, ((0, 2), (1, 16)))
    w_out_delta = centred(key_list[17], (GDN_HEADS * GDN_DIM, D), (SB_HEADS * SB_DIM + GDN_HEADS * GDN_DIM) ** -0.5, 0.125, ((0, 2), (1, 16)))
    return {"tokens": tokens, "ln_gain": ln_gain, "w_query_attn": w_query_attn, "w_key_attn": w_key_attn, "w_value_attn": w_value_attn, "w_query_delta": w_query_delta, "w_key_delta": w_key_delta, "w_value_delta": w_value_delta, "w_beta": w_beta, "w_decay": w_decay, "attn_bias": attn_bias, "decay_log": decay_log, "beta_bias": beta_bias, "log_decay_extra": log_decay_extra, "attn_gain": attn_gain, "delta_gain": delta_gain, "w_out_attn": w_out_attn, "w_out_delta": w_out_delta}


precise = lax.Precision.HIGHEST

def layer_normed(tok_rows, ln_gain):
    values = tok_rows.astype(jnp.float32)
    center = lax.optimization_barrier(jnp.mean(values, axis=-1, keepdims=True))
    spread = lax.optimization_barrier(jnp.mean(jnp.square(values - center), axis=-1, keepdims=True))
    return ((values - center) * lax.rsqrt(spread + 1e-05) * ln_gain).astype(jnp.bfloat16)

def rms_scaled(values, gain):
    return values * lax.rsqrt(lax.optimization_barrier(jnp.mean(jnp.square(values), axis=-1, keepdims=True)) + 1e-06) * gain

def unit_rows(values):
    return values * lax.rsqrt(lax.optimization_barrier(jnp.sum(jnp.square(values), axis=-1, keepdims=True)) + 1e-06)

def stick_block(carry, queries, query_pos, head_bias, key_block, value_block, key_first):
    outputs, log_kept = carry
    key_count = key_block.shape[0]
    heads = queries.shape[1]
    head_width = queries.shape[2]
    scores = jnp.einsum('rhd,khd->hrk', queries.astype(jnp.float32), key_block.reshape(key_count, heads, head_width).astype(jnp.float32))
    scores = scores * head_width ** (-0.5) + head_bias[:, None, None]
    key_pos = key_first + jnp.arange(key_count, dtype=jnp.int32)
    visible = (key_pos[None, :] < query_pos[:, None]) & (key_pos[None, :] >= 0)
    lost = jnp.where(visible[None], -jax.nn.softplus(scores), 0.0)
    between = lax.cumsum(lost, axis=2, reverse=True) - lost + log_kept[:, :, None]
    weights = jnp.where(visible[None], jnp.exp(jax.nn.log_sigmoid(scores) + between), 0.0)
    rounded = lax.optimization_barrier(weights.astype(jnp.bfloat16)).astype(jnp.float32)
    outputs = outputs + jnp.einsum('hrk,khd->hrd', rounded, value_block.reshape(key_count, heads, head_width).astype(jnp.float32))
    return (outputs, log_kept + lax.optimization_barrier(jnp.sum(lost, axis=2)))

def stick_attention(queries, keys, values, head_bias):
    grand_sum = queries.shape[0]
    heads = queries.shape[1]
    head_width = queries.shape[2]
    block = math.gcd(1024, grand_sum)
    blocks = grand_sum // block

    def query_block(index):
        first_pos = (index * block).astype(jnp.int32)
        block_queries = lax.dynamic_slice_in_dim(queries, first_pos, block, 0)
        query_pos = first_pos + jnp.arange(block, dtype=jnp.int32)

        def one_turn(step_index, carry):
            key_first = ((index - step_index) * block).astype(jnp.int32)
            key_block = lax.dynamic_slice_in_dim(keys, key_first, block, 0)
            value_block = lax.dynamic_slice_in_dim(values, key_first, block, 0)
            return stick_block(carry, block_queries, query_pos, head_bias, key_block, value_block, key_first)
        initial_carry = (jnp.zeros((heads, block, head_width), jnp.float32), jnp.zeros((heads, block), jnp.float32))
        outputs, _ = lax.fori_loop(0, index + 1, one_turn, initial_carry)
        return outputs
    results = lax.map(query_block, jnp.arange(blocks, dtype=jnp.int32))
    return jnp.moveaxis(results, 0, 1).reshape(heads, grand_sum, head_width)

def delta_parts(queries, keys, values, beta, decay):
    width = queries.shape[-2]
    key_width = queries.shape[-1]
    decay_sum = jnp.cumsum(decay, axis=-1)
    lower = jnp.tril(jnp.ones((width, width), dtype=bool))
    strict = jnp.tril(jnp.ones((width, width), dtype=bool), -1)
    differ = decay_sum[..., :, None] - decay_sum[..., None, :]
    decay_mask = jnp.where(lower, jnp.exp(jnp.where(lower, differ, 0.0)), 0.0)
    keys_beta = keys * beta[..., None]
    values_beta = values * beta[..., None]
    strict_mat = jnp.where(strict, jnp.einsum('...id,...jd->...ij', keys_beta, keys, precision=precise) * decay_mask, 0.0)
    right_side = jnp.concatenate([keys_beta * jnp.exp(decay_sum)[..., None], values_beta], axis=-1)
    solved = jax.scipy.linalg.solve_triangular(jnp.eye(width, dtype=jnp.float32) + strict_mat, right_side, lower=True)
    solve_keys = solved[..., :key_width]
    solve_values = solved[..., key_width:]
    query_key = jnp.einsum('...id,...jd->...ij', queries, keys, precision=precise) * decay_mask
    query_decayed = queries * jnp.exp(decay_sum)[..., None]
    keys_to_end = keys * jnp.exp(decay_sum[..., -1:] - decay_sum)[..., None]
    block_decay = jnp.exp(decay_sum[..., -1])
    return (solve_keys, solve_values, query_decayed, query_key, keys_to_end, block_decay)

def delta_update(state, block_parts):
    solve_keys, solve_values, query_decayed, query_key, keys_to_end, block_decay = block_parts
    fresh = solve_values - jnp.einsum('hcd,hde->hce', solve_keys, state, precision=precise)
    outputs = jnp.einsum('hcd,hde->hce', query_decayed, state, precision=precise)
    outputs = outputs + jnp.einsum('hij,hje->hie', query_key, fresh, precision=precise)
    state = state * block_decay[:, None, None] + jnp.einsum('hcd,hce->hde', keys_to_end, fresh, precision=precise)
    return (state, outputs)

def delta_attention(queries, keys, values, beta, decay):
    length = queries.shape[0]
    heads = queries.shape[1]
    blocks = length // DBLOCK

    def to_blocks(array):
        return jnp.moveaxis(array.reshape((blocks, DBLOCK) + array.shape[1:]), 2, 0)
    parts = delta_parts(to_blocks(queries), to_blocks(keys), to_blocks(values), to_blocks(beta), to_blocks(decay))
    sequence = tuple((jnp.moveaxis(piece_part, 1, 0) for piece_part in parts))
    start_state = jnp.zeros((heads, queries.shape[2], values.shape[2]), jnp.float32)
    _, outputs = lax.scan(delta_update, start_state, sequence)
    return jnp.moveaxis(outputs, 0, 1).reshape(heads, length, values.shape[2])

def reference(tokens, ln_gain, w_query_attn, w_key_attn, w_value_attn, w_query_delta, w_key_delta, w_value_delta, w_beta, w_decay, attn_bias, decay_log, beta_bias, log_decay_extra, attn_gain, delta_gain, w_out_attn, w_out_delta):
    normed = layer_normed(tokens, ln_gain)
    length = tokens.shape[0]

    def project(weight):
        return jnp.dot(normed.astype(jnp.float32), weight.astype(jnp.float32), preferred_element_type=jnp.float32).astype(jnp.bfloat16)
    attn_query = project(w_query_attn).reshape(length, SB_HEADS, SB_DIM)
    attn_key = project(w_key_attn)
    attn_value = project(w_value_attn)
    delta_query = project(w_query_delta)
    delta_key = project(w_key_delta)
    delta_value = project(w_value_delta)
    beta_pre = project(w_beta)
    decay_pre = project(w_decay)
    attn_raw = stick_attention(attn_query, attn_key, attn_value, attn_bias)
    attn_mixed = rms_scaled(attn_raw, attn_gain).astype(jnp.bfloat16)
    queries = unit_rows(jax.nn.silu(delta_query.astype(jnp.float32)).reshape(length, GDN_HEADS, GDN_DIM)) * GDN_DIM ** (-0.5)
    keys = unit_rows(jax.nn.silu(delta_key.astype(jnp.float32)).reshape(length, GDN_HEADS, GDN_DIM))
    values = jax.nn.silu(delta_value.astype(jnp.float32)).reshape(length, GDN_HEADS, GDN_DIM)
    beta = jax.nn.sigmoid(beta_pre.astype(jnp.float32) + beta_bias)
    decay = -jnp.exp(decay_log) * jax.nn.softplus(decay_pre.astype(jnp.float32)) + log_decay_extra
    delta_raw = delta_attention(queries, keys, values, beta, decay)
    delta_mixed = rms_scaled(delta_raw, delta_gain).astype(jnp.bfloat16)
    attn_group = SB_HEADS // N_TP
    delta_group = GDN_HEADS // N_TP
    summed = jnp.zeros((length, w_out_attn.shape[1]), jnp.float32)
    for group in range(N_TP):
        attn_cols = jnp.transpose(attn_mixed[group * attn_group:(group + 1) * attn_group], (1, 0, 2)).reshape(length, attn_group * SB_DIM)
        delta_cols = jnp.transpose(delta_mixed[group * delta_group:(group + 1) * delta_group], (1, 0, 2)).reshape(length, delta_group * GDN_DIM)
        partial_sum = jnp.dot(attn_cols.astype(jnp.float32), w_out_attn[group * attn_group * SB_DIM:(group + 1) * attn_group * SB_DIM].astype(jnp.float32), preferred_element_type=jnp.float32)
        partial_sum = partial_sum + jnp.dot(delta_cols.astype(jnp.float32), w_out_delta[group * delta_group * GDN_DIM:(group + 1) * delta_group * GDN_DIM].astype(jnp.float32), preferred_element_type=jnp.float32)
        summed = summed + lax.optimization_barrier(partial_sum.astype(jnp.bfloat16)).astype(jnp.float32)
    return summed.astype(jnp.bfloat16)
```

```python
import functools

import jax
import jax.numpy as jnp
from jax import lax
from jax.experimental import pallas as pl
from jax.experimental.pallas import tpu as pltpu
from jax.sharding import PartitionSpec as P

SB_DIM = 64
GDN_DIM = 128

VMEM = pltpu.VMEM
SMEM = pltpu.SMEM


def layer_normed(tok_rows, ln_gain):
    values = tok_rows.astype(jnp.float32)
    center = jnp.mean(values, axis=-1, keepdims=True)
    spread = jnp.mean(jnp.square(values - center), axis=-1, keepdims=True)
    return ((values - center) * lax.rsqrt(spread + 1e-05) * ln_gain).astype(jnp.bfloat16)


def unit_rows(values):
    return values * lax.rsqrt(jnp.sum(jnp.square(values), axis=-1, keepdims=True) + 1e-06)


def split2(a):
    high = a.astype(jnp.bfloat16)
    return high, (a - high.astype(jnp.float32)).astype(jnp.bfloat16)


def dot_f32(a, b, dims):
    return lax.dot_general(a, b, (dims, ((), ())), preferred_element_type=jnp.float32)


NN = ((1,), (0,))
NT = ((1,), (1,))
TN = ((0,), (0,))


def dot3(a, b, dims=NN):
    ah, al = split2(a)
    bh, bl = split2(b)
    return dot_f32(ah, bh, dims) + (dot_f32(ah, bl, dims) + dot_f32(al, bh, dims))


def stick_kernel(rows, part, off_ref, bias_ref, gain_ref, got_ref, out_ref):
    index = pl.program_id(0)
    queries = got_ref[index, rows : rows + part, :]
    bias = bias_ref[0]
    later = lax.broadcasted_iota(jnp.int32, (rows, rows), 0) > lax.broadcasted_iota(
        jnp.int32, (rows, rows), 1
    )
    later = jnp.where(later, 1.0, 0.0).astype(jnp.bfloat16)

    def turn(block, carry, visible=None):
        acc, kept = carry
        both = got_ref[block, 0:rows, :]
        z = dot_f32(queries, both, NT) * SB_DIM ** (-0.5) + bias
        tail = jnp.log(1.0 + jnp.exp(-jnp.abs(z)))
        lost = -(jnp.maximum(z, 0.0) + tail)
        if visible is not None:
            lost = jnp.where(visible, lost, 0.0)
        high, low = split2(lost)
        between = dot_f32(high, later, NN) + dot_f32(low, later, NN)
        weight = jnp.exp((jnp.minimum(z, 0.0) - tail) + between + kept)
        if visible is not None:
            weight = jnp.where(visible, weight, 0.0)
        acc = acc + dot_f32(weight.astype(jnp.bfloat16), both, NN)
        return acc, kept + (between[:, 0:1] + lost[:, 0:1])

    seen = lax.broadcasted_iota(jnp.int32, (part, rows), 1) < lax.broadcasted_iota(
        jnp.int32, (part, rows), 0
    ) + off_ref[0]
    carry = (jnp.zeros((part, 2 * SB_DIM), jnp.float32), jnp.zeros((part, 1), jnp.float32))
    carry = turn(index, carry, seen)
    odd = lax.rem(index, 2)
    carry = lax.fori_loop(0, odd, lambda step, c: turn(index - 1, c), carry)

    def pair(step, c):
        last = index - odd - 1 - 2 * step
        return turn(last - 1, turn(last, c))

    acc, _ = lax.fori_loop(0, lax.div(index, 2), pair, carry)
    lane = lax.broadcasted_iota(jnp.int32, acc.shape, 1)
    square = jnp.sum(jnp.where(lane >= SB_DIM, acc * acc, 0.0), axis=-1, keepdims=True)
    out = acc * lax.rsqrt(square * (1.0 / SB_DIM) + 1e-06) * gain_ref[...]
    out_ref[0] = out.astype(jnp.bfloat16)


def delta_kernel(q_ref, k_ref, v_ref, col_ref, row_ref, from_ref, own_ref, map_ref):
    rows, width = q_ref.shape
    silu = lambda ref: jax.nn.silu(ref[...].astype(jnp.float32))
    query = unit_rows(silu(q_ref)) * width ** (-0.5)
    key = unit_rows(silu(k_ref))
    value = silu(v_ref)
    beta = col_ref[0, :, 0:1]
    g_col = col_ref[0, :, 1:2]
    g_row = row_ref[0]
    ii = lax.broadcasted_iota(jnp.int32, (rows, rows), 0)
    jj = lax.broadcasted_iota(jnp.int32, (rows, rows), 1)
    lower = ii >= jj
    sum_col = jnp.sum(jnp.where(lower, g_row, 0.0), axis=1, keepdims=True)
    sum_row = jnp.sum(jnp.where(ii <= jj, g_col, 0.0), axis=0, keepdims=True)
    end = sum_col[rows - 1 : rows, :]
    decay_mask = jnp.where(lower, jnp.exp(jnp.where(lower, sum_col - sum_row, 0.0)), 0.0)
    key_beta = key * beta
    strict = jnp.where(ii > jj, dot3(key_beta, key, NT) * decay_mask, 0.0)
    inverse = jnp.where(
        ii == jj, 1.0, jnp.where((ii >> 1) == (jj >> 1), -strict, 0.0)
    )
    level = 1
    while (1 << level) < rows:
        joined = (ii >> (level + 1)) == (jj >> (level + 1))
        apart = (ii >> level) != (jj >> level)
        corner = jnp.where(joined & apart, strict, 0.0)
        inverse = inverse - dot3(dot3(inverse, corner), inverse)
        level += 1
    grown = jnp.exp(sum_col)
    solved = dot3(inverse, jnp.concatenate([key_beta * grown, value * beta], axis=1))
    query_key = dot3(query, key, NT) * decay_mask
    mixed = dot3(query_key, solved)
    from_ref[...] = query * grown - mixed[:, :width]
    own_ref[...] = mixed[:, width:]
    map_ref[0] = dot3(key * jnp.exp(end - sum_col), solved, TN).astype(jnp.bfloat16)


def state_kernel(heads, pos_ref, decay_ref, gain_ref, maps_ref, from_ref, own_ref, out_ref):
    width = gain_ref.shape[1]

    def turn(block, states):
        new = []
        for head, state in enumerate(states):
            high, low = split2(state)
            both = maps_ref[block, head]
            taken = both[:, :width]
            moved = dot_f32(taken, high, NN) + dot_f32(taken, low, NN)
            new.append(
                state * decay_ref[block, head] - moved + both[:, width:].astype(jnp.float32)
            )
        return tuple(new)

    zero = jnp.zeros((width, width), jnp.float32)
    states = lax.fori_loop(0, pos_ref[0], turn, (zero,) * heads)
    for head, state in enumerate(states):
        cols = slice(head * width, (head + 1) * width)
        raw = dot3(from_ref[:, cols], state) + own_ref[:, cols]
        scale = lax.rsqrt(jnp.mean(raw * raw, axis=-1, keepdims=True) + 1e-06)
        out_ref[:, cols] = (raw * scale * gain_ref[...]).astype(jnp.bfloat16)


def local(
    tokens,
    ln_gain,
    w_query_attn,
    w_key_attn,
    w_value_attn,
    w_query_delta,
    w_key_delta,
    w_value_delta,
    w_beta,
    w_decay,
    attn_bias,
    decay_log,
    beta_bias,
    log_decay_extra,
    attn_gain,
    delta_gain,
    w_out_attn,
    w_out_delta,
):
    rows = tokens.shape[0]
    sp_size = lax.axis_size("sp")
    tp_pos = lax.axis_index("tp")
    sp_pos = lax.axis_index("sp")
    heads = w_query_attn.shape[1] // SB_DIM
    delta_heads = w_query_delta.shape[1] // GDN_DIM
    group = sp_size // heads
    part = rows // group
    depth = w_query_attn.shape[0]

    w_delta = jnp.concatenate([w_query_delta, w_key_delta, w_value_delta], axis=1)
    w_pairs = jnp.concatenate(
        [w_key_attn.reshape(depth, heads, SB_DIM), w_value_attn.reshape(depth, heads, SB_DIM)],
        axis=2,
    ).reshape(depth, 2 * heads * SB_DIM)
    w_attn = jnp.concatenate([w_pairs, w_query_attn], axis=1)
    w_delta = lax.all_gather(w_delta, "sp", axis=0, tiled=True)
    w_attn = lax.all_gather(w_attn, "sp", axis=0, tiled=True)

    normed = layer_normed(tokens, ln_gain)
    project = lambda w: jnp.dot(normed, w, preferred_element_type=jnp.float32).astype(jnp.bfloat16)

    first = tp_pos * delta_heads
    mine = lambda a, axis: lax.dynamic_slice_in_dim(a, first, delta_heads, axis)
    gates = project(jnp.concatenate([mine(w_beta, 1), mine(w_decay, 1)], axis=1))
    gates = gates.astype(jnp.float32)
    beta = jax.nn.sigmoid(gates[:, :delta_heads] + mine(beta_bias, 0))
    rates = jnp.exp(mine(decay_log, 0))
    decay = -rates * jax.nn.softplus(gates[:, delta_heads:]) + log_decay_extra
    block_decay = lax.all_gather(jnp.exp(jnp.sum(decay, axis=0)), "sp", axis=0)
    cols = jnp.transpose(jnp.stack([beta, decay], axis=2), (1, 0, 2))
    g_rows = jnp.transpose(decay)[:, None, :]

    delta_all = project(w_delta)
    head_cols = lambda base: pl.BlockSpec((rows, GDN_DIM), lambda h: (0, base + h))
    wide = delta_heads * GDN_DIM
    from_state, own, maps = pl.pallas_call(
        delta_kernel,
        grid=(delta_heads,),
        in_specs=[
            head_cols(0),
            head_cols(delta_heads),
            head_cols(2 * delta_heads),
            pl.BlockSpec((1, rows, 2), lambda h: (h, 0, 0)),
            pl.BlockSpec((1, 1, rows), lambda h: (h, 0, 0)),
        ],
        out_specs=[
            head_cols(0),
            head_cols(0),
            pl.BlockSpec((1, GDN_DIM, 2 * GDN_DIM), lambda h: (h, 0, 0)),
        ],
        out_shape=[
            jax.ShapeDtypeStruct((rows, wide), jnp.float32),
            jax.ShapeDtypeStruct((rows, wide), jnp.float32),
            jax.ShapeDtypeStruct((delta_heads, GDN_DIM, 2 * GDN_DIM), jnp.bfloat16),
        ],
        cost_estimate=pl.CostEstimate(
            flops=delta_heads * 120 * rows**3, bytes_accessed=4 * rows * wide, transcendentals=0
        ),
        name="delta_blocks",
    )(delta_all, delta_all, delta_all, cols, g_rows)
    maps = lax.all_gather(maps, "sp", axis=0)

    attn_all = project(w_attn)
    pair_wide = 2 * heads * SB_DIM
    pairs = jnp.transpose(attn_all[:, :pair_wide].reshape(rows, heads, 2 * SB_DIM), (1, 0, 2))
    queries = attn_all[:, pair_wide:].reshape(group, part, heads, SB_DIM)
    queries = jnp.transpose(queries, (2, 0, 1, 3))
    queries = jnp.pad(queries, ((0, 0), (0, 0), (0, 0), (0, SB_DIM)))
    pairs = jnp.broadcast_to(pairs[:, None], (heads, group, rows, 2 * SB_DIM))
    sent = jnp.concatenate([pairs, queries], axis=2).reshape(sp_size, rows + part, 2 * SB_DIM)
    got = lax.all_to_all(sent, "sp", 0, 0, tiled=True)
    bias = lax.dynamic_slice_in_dim(attn_bias, tp_pos * heads + sp_pos // group, 1, 0)
    offset = (lax.rem(sp_pos, group) * part).astype(jnp.int32)[None]
    gain = jnp.concatenate([jnp.zeros_like(attn_gain), attn_gain])[None]
    mixed = pl.pallas_call(
        functools.partial(stick_kernel, rows, part),
        grid=(sp_size,),
        in_specs=[
            pl.BlockSpec(memory_space=SMEM),
            pl.BlockSpec(memory_space=SMEM),
            pl.BlockSpec(memory_space=VMEM),
            pl.BlockSpec(memory_space=VMEM),
        ],
        out_specs=pl.BlockSpec((1, part, 2 * SB_DIM), lambda i: (i, 0, 0)),
        out_shape=jax.ShapeDtypeStruct((sp_size, part, 2 * SB_DIM), jnp.bfloat16),
        cost_estimate=pl.CostEstimate(
            flops=sp_size * sp_size * rows * part * 20000,
            bytes_accessed=sp_size * rows * 512,
            transcendentals=0,
        ),
        name="stick_attention",
    )(offset, bias, gain, got)
    back = lax.all_to_all(mixed[:, :, SB_DIM:], "sp", 0, 0, tiled=True)
    back = back.reshape(heads, group, part, SB_DIM)
    attn_cols = jnp.transpose(back, (1, 2, 0, 3)).reshape(rows, heads * SB_DIM)

    delta_cols = pl.pallas_call(
        functools.partial(state_kernel, delta_heads),
        in_specs=[pl.BlockSpec(memory_space=SMEM)] * 2 + [pl.BlockSpec(memory_space=VMEM)] * 4,
        out_specs=pl.BlockSpec(memory_space=VMEM),
        out_shape=jax.ShapeDtypeStruct((rows, wide), jnp.bfloat16),
        cost_estimate=pl.CostEstimate(
            flops=sp_size * wide * GDN_DIM * 10000, bytes_accessed=8 * rows * wide, transcendentals=0
        ),
        name="delta_state",
    )(sp_pos.astype(jnp.int32)[None], block_decay, delta_gain[None], maps, from_state, own)

    w_out = lax.all_gather(
        jnp.concatenate([w_out_attn, w_out_delta], axis=0), "sp", axis=1, tiled=True
    )
    joined = jnp.concatenate([attn_cols, delta_cols], axis=1)
    result = jnp.dot(joined, w_out, preferred_element_type=jnp.float32).astype(jnp.bfloat16)
    return lax.psum_scatter(result, "tp", scatter_dimension=0, tiled=True)


def solution(mesh):
    in_specs = (
        P("sp", None),
        P(),
        P("sp", "tp"),
        P("sp", "tp"),
        P("sp", "tp"),
        P("sp", "tp"),
        P("sp", "tp"),
        P("sp", "tp"),
        P(),
        P(),
        P(),
        P(),
        P(),
        P("sp", "tp"),
        P(),
        P(),
        P("tp", "sp"),
        P("tp", "sp"),
    )
    out_specs = P(("sp", "tp"), None)
    return jax.shard_map(local, mesh=mesh, in_specs=in_specs, out_specs=out_specs, check_vma=False)
```
